32 devices in a mesh: row: 8 (over z, core), col: 4 (over y, x).
Axes of the slice: x: 2, y: 2, z: 4, core: 2. Of those that a mesh axis runs over, the one named last changes fastest.
Arguments:
- streams: bfloat16 [3, 1, 4096, 512], P(None, None, ('row', 'col')), may hold values from -6 to 6
- filter_taps: float32 [2, 4096, 512], P(None, ('row', 'col')), may hold values from -4 to 4
- short_taps: float32 [3, 3, 512], replicated, may hold values from -3 to 3
- skip_gain: float32 [512], replicated, may hold values from -3 to 3
- out_weight: bfloat16 [512, 4096], replicated, may hold values from -0.25 to 0.25
Outputs:
- projected: bfloat16 [1, 4096, 4096], P(None, ('row', 'col'))
The draws below stay inside these ranges and needn't reach their ends.
All inputs are finite; a program needn't handle non-finite values.
Results may differ from the reference program's by a relative error of at most 0.0049.
Values may be sent and summed in bfloat16 or wider, within the bound.
A program may use at most 64 MiB of HBM per device.

```python
import math
import jax
import jax.numpy as jnp
from jax import lax

WIDTH = 4096
CHANNELS = 512
SEQUENCES = 1
LENGTH = 4096


def draw_filter_taps(key, part):
    subkeys = jax.random.split(jax.random.fold_in(key, 11), 4)
    roughness = jax.random.truncated_normal(subkeys[0], -4.0, 4.0, (2, LENGTH, CHANNELS), jnp.float32)
    selector = jax.random.uniform(subkeys[1], (2, 1, CHANNELS), jnp.float32)
    slow_reach = LENGTH * jnp.exp(jax.random.uniform(subkeys[2], (2, 1, CHANNELS), jnp.float32, math.log(0.5), math.log(4.0)))
    fast_reach = jnp.exp(jax.random.uniform(subkeys[3], (2, 1, CHANNELS), jnp.float32, math.log(30.0), math.log(50.0)))
    share_slow = 0.5
    chosen_reach = jnp.where(selector < share_slow, slow_reach, fast_reach)
    offsets = jnp.arange(LENGTH, dtype=jnp.float32)
    distance = jnp.stack([offsets, LENGTH - offsets])[:, :, None]
    envelope = jnp.exp(-distance / chosen_reach)
    magnitude = jnp.sqrt(jnp.sum(jnp.square(envelope), axis=(0, 1), keepdims=True))
    return roughness * envelope / magnitude


def steps_of(key, dims, shards, smallest, largest):
    def one(position, shards_of):
        steps = jax.random.uniform(jax.random.fold_in(jax.random.fold_in(key, 6), position), (shards_of,), jnp.float32, smallest / len(shards), largest / len(shards))
        return jnp.repeat(jnp.exp(steps), dims[position] // shards_of).reshape((-1,) + (1,) * (len(dims) - position - 1))

    level = one(*shards[0])
    for cut in shards[1:]:
        level = level * one(*cut)
    return level


def normal_values(stream_key, shape, deviation, most, cuts=(), kind=jnp.bfloat16):
    array = jax.random.normal(stream_key, shape, jnp.float32) * deviation
    if len(cuts) > 0:
        array = steps_of(stream_key, shape, cuts, -0.22, 0.18) * array
    return jnp.clip(array, min=-most, max=most).astype(kind)


def setup_inputs(seed: int = 0) -> dict:
    seeds = jax.random.split(jax.random.key(seed), 6)
    streams = normal_values(seeds[0], (3, SEQUENCES, LENGTH, CHANNELS), 1.0, 6.0, ((2, 32),))
    filter_taps = draw_filter_taps(jax.random.fold_in(seeds[5], 71), 0)
    short_taps = normal_values(seeds[2], (3, 3, CHANNELS), 0.577, 3.0, (), jnp.float32)
    skip_gain = normal_values(seeds[3], (CHANNELS,), 0.5, 3.0, (), jnp.float32)
    out_weight = normal_values(seeds[4], (CHANNELS, WIDTH), CHANNELS ** -0.5, 0.25)
    return {"streams": streams, "filter_taps": filter_taps, "short_taps": short_taps, "skip_gain": skip_gain, "out_weight": out_weight}


EPSILON = 1e-06

def smooth_streams(streams, short_taps):
    widened = streams.astype(jnp.float32)
    padded = jnp.pad(widened, ((0, 0), (0, 0), (1, 1), (0, 0)))
    return short_taps[:, 0][:, None, None, :] * padded[:, :, :-2] + short_taps[:, 1][:, None, None, :] * padded[:, :, 1:-1] + short_taps[:, 2][:, None, None, :] * padded[:, :, 2:]

def reference(streams, filter_taps, short_taps, skip_gain, out_weight):
    smoothed = smooth_streams(streams, short_taps)
    gated = smoothed[2] * smoothed[1]
    kernel_spectrum = jnp.fft.rfft(filter_taps.reshape(2 * LENGTH, CHANNELS), axis=0)

    def one_sequence(operands):
        gated_rows, gate_rows = operands
        spectrum = jnp.fft.rfft(gated_rows, n=2 * LENGTH, axis=0) * kernel_spectrum
        convolved = jnp.fft.irfft(spectrum, n=2 * LENGTH, axis=0)[:LENGTH]
        mixed = ((convolved + skip_gain * gated_rows) * gate_rows).astype(jnp.bfloat16)
        mean_square = lax.optimization_barrier(jnp.mean(jnp.square(mixed.astype(jnp.float32)), axis=-1, keepdims=True))
        product = jnp.dot(mixed, out_weight, preferred_element_type=jnp.float32)
        return (product * lax.rsqrt(mean_square + EPSILON)).astype(jnp.bfloat16)
    return lax.map(one_sequence, (gated, smoothed[0]))
```

```python
import functools
import math

import jax
import jax.numpy as jnp
import numpy as np
from jax import lax
from jax.experimental import pallas as pl
from jax.experimental.pallas import tpu as pltpu
from jax.sharding import PartitionSpec as P

HIGHEST_PRECISION = lax.Precision.HIGHEST
EPSILON = 1e-06


def with_halo(cells, sides, width):
    for axis, dim in sides:
        count = lax.axis_size(axis)
        ends = count - 1
        head = lax.slice_in_dim(cells, 0, width, axis=dim)
        tail = lax.slice_in_dim(cells, cells.shape[dim] - width, cells.shape[dim], axis=dim)
        cells = jnp.concatenate(
            [
                lax.ppermute(tail, axis, [(i, (i + 1) % count) for i in range(ends)]),
                cells,
                lax.ppermute(head, axis, [((i + 1) % count, i) for i in range(ends)]),
            ],
            axis=dim,
        )
    return cells


def unit_circle(numerator, period):
    angles = 2.0 * math.pi / period * (numerator % period).astype(jnp.float32)
    return (jnp.cos(angles), jnp.sin(angles))


def complex_times(left_real, left_imag, right_real, right_imag):
    return (
        left_real * right_real - left_imag * right_imag,
        left_real * right_imag + left_imag * right_real,
    )


def complex_einsum(formula, matrix_real, matrix_imag, operand_real, operand_imag):

    def single(matrix, operand):
        return jnp.einsum(formula, matrix, operand, precision=HIGHEST_PRECISION)

    return (
        single(matrix_real, operand_real) - single(matrix_imag, operand_imag),
        single(matrix_real, operand_imag) + single(matrix_imag, operand_real),
    )


def sequence_offsets(column_count, positions):
    blocks = jnp.arange(column_count, dtype=jnp.int32)
    within = jnp.arange(positions, dtype=jnp.int32)
    return (blocks, within, positions * blocks[:, None] + within[None, :])


def forward_rows(real_part, imag_part, frequencies, length):
    column_count, positions = (real_part.shape[1], real_part.shape[4])
    blocks, within, offsets = sequence_offsets(column_count, positions)
    cos_table, sin_table = unit_circle(frequencies[:, None, None] * offsets[None], length)
    real_part, imag_part = complex_times(
        real_part, imag_part, cos_table[:, :, None, None, :], -sin_table[:, :, None, None, :]
    )
    cos_table, sin_table = unit_circle(blocks[:, None] * blocks[None, :], column_count)
    real_part, imag_part = complex_einsum(
        "mc,rcbhj->rmbhj", cos_table, -sin_table, real_part, imag_part
    )
    cos_table, sin_table = unit_circle(blocks[:, None] * within[None, :], column_count * positions)
    real_part, imag_part = complex_times(
        real_part, imag_part, cos_table[None, :, None, None, :], -sin_table[None, :, None, None, :]
    )
    cos_table, sin_table = unit_circle(within[:, None] * within[None, :], positions)
    return complex_einsum("nj,rmbhj->rmbhn", cos_table, -sin_table, real_part, imag_part)


def inverse_rows(real_part, imag_part, frequencies, length):
    column_count, positions = (real_part.shape[1], real_part.shape[4])
    blocks, within, offsets = sequence_offsets(column_count, positions)
    cos_table, sin_table = unit_circle(within[:, None] * within[None, :], positions)
    real_part, imag_part = complex_einsum(
        "jn,rmbhn->rmbhj", cos_table, sin_table, real_part, imag_part
    )
    cos_table, sin_table = unit_circle(blocks[:, None] * within[None, :], column_count * positions)
    real_part, imag_part = complex_times(
        real_part, imag_part, cos_table[None, :, None, None, :], sin_table[None, :, None, None, :]
    )
    cos_table, sin_table = unit_circle(blocks[:, None] * blocks[None, :], column_count)
    real_part, imag_part = complex_einsum(
        "cm,rmbhj->rcbhj", cos_table, sin_table, real_part, imag_part
    )
    cos_table, sin_table = unit_circle(frequencies[:, None, None] * offsets[None], length)
    return complex_times(
        real_part, imag_part, cos_table[:, :, None, None, :], sin_table[:, :, None, None, :]
    )


def row_transform(operand, frequencies, sources, period):
    cos_table, sin_table = unit_circle(frequencies[:, None] * sources[None, :], period)
    imag_matrix = -sin_table
    flipped = unit_circle(period // 2 * sources[None, :], period)[0]
    imag_matrix = jnp.where(frequencies[:, None] == 0, flipped, imag_matrix)
    return (
        jnp.dot(cos_table, operand, precision=HIGHEST_PRECISION),
        jnp.dot(imag_matrix, operand, precision=HIGHEST_PRECISION),
    )


def row_inverse(real_part, imag_part, frequencies, rows_count, period, length):
    targets = jnp.arange(rows_count, dtype=jnp.int32)
    cos_table, sin_table = unit_circle(targets[:, None] * frequencies[None, :], period)
    real_matrix = cos_table / length
    imag_matrix = -sin_table / length
    flipped = unit_circle(period // 2 * targets[:, None], period)[0]
    head_row = frequencies[None, :] == 0
    real_matrix = jnp.where(head_row, 1.0, 2.0 * cos_table) / length
    imag_matrix = jnp.where(head_row, flipped, -2.0 * sin_table) / length
    return jnp.dot(real_matrix, real_part, precision=HIGHEST_PRECISION) + jnp.dot(
        imag_matrix, imag_part, precision=HIGHEST_PRECISION
    )


def unpack_head(real_part, imag_part, first_device):
    head_row = (jnp.arange(real_part.shape[0]) == 0)[:, None, None, None, None] & first_device
    extra_row = jnp.where(first_device, imag_part[:1], 0.0)
    cleared = jnp.where(head_row, 0.0, imag_part)
    return (
        jnp.concatenate([real_part, extra_row], axis=0),
        jnp.concatenate([cleared, jnp.zeros_like(extra_row)], axis=0),
    )


def pack_head(real_part, imag_part, first_device):
    head_imag = jnp.where(first_device, real_part[-1:], imag_part[:1])
    return (real_part[:-1], jnp.concatenate([head_imag, imag_part[1:-1]], axis=0))


def spectral_middle(signal, kernel, sequences, positions, share, column_index, send_out, send_back):
    rows_count = signal.shape[0]
    period = 2 * rows_count
    column_count = lax.axis_size("col")
    length = period * column_count * positions
    local_rows = rows_count // column_count
    frequencies = jnp.arange(rows_count, dtype=jnp.int32)
    signal_sources = jnp.arange(rows_count, dtype=jnp.int32)
    kernel_index = jnp.arange(period, dtype=jnp.int32)
    kernel_sources = kernel_index % 2 * rows_count + kernel_index // 2
    signal_real, signal_imag = row_transform(signal, frequencies, signal_sources, period)
    kernel_real, kernel_imag = row_transform(kernel, frequencies, kernel_sources, period)
    moved = send_out(
        signal_real[:, None], signal_imag[:, None], kernel_real[:, None], kernel_imag[:, None]
    )
    signal_shape = (local_rows, column_count, sequences, share, positions)
    kernel_shape = (local_rows, column_count, 1, share, positions)
    signal_real = moved[0].reshape(signal_shape)
    signal_imag = moved[1].reshape(signal_shape)
    kernel_real = moved[2].reshape(kernel_shape)
    kernel_imag = moved[3].reshape(kernel_shape)
    local_freq = column_index * local_rows + jnp.arange(local_rows, dtype=jnp.int32)
    first_device = column_index == 0
    signal_real, signal_imag = unpack_head(signal_real, signal_imag, first_device)
    kernel_real, kernel_imag = unpack_head(kernel_real, kernel_imag, first_device)
    local_freq = jnp.concatenate([local_freq, jnp.full((1,), rows_count, jnp.int32)])
    signal_real, signal_imag = forward_rows(signal_real, signal_imag, local_freq, length)
    kernel_real, kernel_imag = forward_rows(kernel_real, kernel_imag, local_freq, length)
    product_real, product_imag = complex_times(signal_real, signal_imag, kernel_real, kernel_imag)
    product_real, product_imag = inverse_rows(product_real, product_imag, local_freq, length)
    product_real, product_imag = pack_head(product_real, product_imag, first_device)
    returned = send_back(product_real, product_imag)
    columns = sequences * share * positions
    return row_inverse(
        returned[0].reshape(rows_count, columns),
        returned[1].reshape(rows_count, columns),
        frequencies,
        rows_count,
        period,
        length,
    )


def local(streams, filter_taps, short_taps, skip_gain, out_weight):
    sequences, positions, channels = (streams.shape[1], streams.shape[2], streams.shape[3])
    rows_count = lax.axis_size("row")
    share = channels // rows_count
    column_index = lax.axis_index("col")
    padded = with_halo(streams, ((("row", "col"), 2),), 1)
    smoothed = (
        short_taps[:, 0][:, None, None, :] * padded[:, :, :-2]
        + short_taps[:, 1][:, None, None, :] * padded[:, :, 1:-1]
        + short_taps[:, 2][:, None, None, :] * padded[:, :, 2:]
    )
    gated = smoothed[2] * smoothed[1]
    gated_lanes = jnp.transpose(gated, (0, 2, 1))[None]
    taps_lanes = jnp.transpose(filter_taps, (0, 2, 1))[:, None]
    by_channel, kernel_channel = (
        lax.all_to_all(gated_lanes, "row", split_axis=2, concat_axis=0, tiled=True),
        lax.all_to_all(taps_lanes, "row", split_axis=2, concat_axis=0, tiled=True),
    )
    signal = by_channel.reshape(rows_count, sequences * share * positions)
    kernel = kernel_channel.reshape(2 * rows_count, share * positions)

    def send_out(part_one, part_two, part_three, part_four):
        return (
            lax.all_to_all(part_one, "col", split_axis=0, concat_axis=1, tiled=True),
            lax.all_to_all(part_two, "col", split_axis=0, concat_axis=1, tiled=True),
            lax.all_to_all(part_three, "col", split_axis=0, concat_axis=1, tiled=True),
            lax.all_to_all(part_four, "col", split_axis=0, concat_axis=1, tiled=True),
        )

    def send_back(part_one, part_two):
        return (
            lax.all_to_all(part_one, "col", split_axis=1, concat_axis=0, tiled=True),
            lax.all_to_all(part_two, "col", split_axis=1, concat_axis=0, tiled=True),
        )

    spatial = spectral_middle(
        signal, kernel, sequences, positions, share, column_index, send_out, send_back
    )
    returned = lax.all_to_all(
        spatial.reshape(rows_count, sequences, share, positions),
        "row",
        split_axis=0,
        concat_axis=2,
        tiled=True,
    )
    convolved = jnp.transpose(returned[0], (0, 2, 1))
    mixed = ((convolved + skip_gain * gated) * smoothed[0]).astype(jnp.bfloat16)
    flattened = mixed.reshape(sequences * positions, channels)
    mean_square = jnp.mean(jnp.square(flattened.astype(jnp.float32)), axis=-1, keepdims=True)
    product = jnp.dot(flattened, out_weight, preferred_element_type=jnp.float32)
    scaled = (product * lax.rsqrt(mean_square + EPSILON)).astype(jnp.bfloat16)
    return scaled.reshape(sequences, positions, out_weight.shape[1])


def split_pair(value):
    high = value.astype(jnp.bfloat16)
    return high, (value - high.astype(jnp.float32)).astype(jnp.bfloat16)


def split_pair_host(table):
    table = np.asarray(table, np.float32)
    high = table.astype(jnp.bfloat16)
    return high, (table - high.astype(np.float32)).astype(jnp.bfloat16)


def host_tables(devices, share, positions):
    blocks = 2 * devices
    length = blocks * positions
    first = np.arange(devices + 1)
    source = np.arange(devices)
    angle = 2.0 * np.pi / blocks * (first[:, None] * source[None, :] % blocks)
    rows = np.concatenate([np.cos(angle), -np.sin(angle[1:devices])])
    outer = np.kron(rows, np.eye(share))
    within = np.arange(positions)
    angle = 2.0 * np.pi / length * (first[:, None] * within[None, :] % length)
    twiddle = np.stack([np.cos(angle), np.sin(angle)])[:, :, None, :].astype(np.float32)
    angle = 2.0 * np.pi / positions * (within[:, None] * within[None, :] % positions)
    cos_table, sin_table = np.cos(angle), np.sin(angle)
    inner = np.block([[cos_table, -sin_table], [sin_table, cos_table]])
    return (*split_pair_host(outer), *split_pair_host(inner), twiddle)


def dot32(left, right, dims=((1,), (0,))):
    return lax.dot_general(left, right, (dims, ((), ())), preferred_element_type=jnp.float32)


def whole_kernel(
    axes, sizes, streams_hbm, taps_hbm, short_ref, gain_ref, weight_hbm, outer_high_hbm, outer_low_hbm,
    inner_high_ref, inner_low_ref, twiddle_ref, out_ref,
    streams, taps, weight, outer_high, outer_low, halo_before, halo_after,
    taps_send, taps_recv, gated_send, gated_recv, back_send, back_recv,
    local_sems, halo_sems, send_sems, recv_sems,
):
    devices, share, positions, channels = sizes
    columns = lax.axis_size(axes[1])
    me = lax.axis_index(axes[0]) * columns + lax.axis_index(axes[1])
    mesh_id = pl.DeviceIdType.MESH

    def place(device):
        return (lax.div(device, columns), lax.rem(device, columns))

    def partner(step):
        return lax.rem(me + step, devices)

    loads = [
        pltpu.make_async_copy(source, target, local_sems.at[i])
        for i, (source, target) in enumerate(
            [
                (taps_hbm, taps),
                (streams_hbm, streams),
                (outer_high_hbm, outer_high),
                (outer_low_hbm, outer_low),
                (weight_hbm, weight),
            ]
        )
    ]
    for load in loads:
        load.start()
    barrier = pltpu.get_barrier_semaphore()
    for step in range(1, devices):
        pl.semaphore_signal(barrier, inc=1, device_id=place(partner(step)), device_id_type=mesh_id)

    loads[0].wait()
    for half in range(2):
        turned = jnp.transpose(taps[half]).astype(jnp.bfloat16)
        taps_send[half] = turned.reshape(devices, share, positions)
    taps_recv[:, me] = taps_send[:, me]
    pl.semaphore_wait(barrier, devices - 1)

    edge = halo_before.shape[1]
    halo_copies = [
        pltpu.make_async_remote_copy(
            src_ref=streams_hbm.at[:, pl.ds(positions - edge, edge)],
            dst_ref=halo_before,
            send_sem=halo_sems.at[0],
            recv_sem=halo_sems.at[1],
            device_id=place(partner(1)),
            device_id_type=mesh_id,
        ),
        pltpu.make_async_remote_copy(
            src_ref=streams_hbm.at[:, pl.ds(0, edge)],
            dst_ref=halo_after,
            send_sem=halo_sems.at[2],
            recv_sem=halo_sems.at[3],
            device_id=place(partner(devices - 1)),
            device_id_type=mesh_id,
        ),
    ]
    for copy in halo_copies:
        copy.start()

    def exchange(kind, source, target):
        copies = []
        for step in range(1, devices):
            device = partner(step)
            copies.append(
                pltpu.make_async_remote_copy(
                    src_ref=source(device),
                    dst_ref=target,
                    send_sem=send_sems.at[kind, step],
                    recv_sem=recv_sems.at[kind, step],
                    device_id=place(device),
                    device_id_type=mesh_id,
                )
            )
        for copy in copies:
            copy.start()
        return copies

    taps_copies = exchange(0, lambda device: taps_send.at[:, device], taps_recv.at[:, me])

    loads[1].wait()
    for copy in halo_copies:
        copy.wait()
    row = lax.broadcasted_iota(jnp.int32, (positions, channels), 0)
    smoothed = []
    for s in range(3):
        middle = streams[s].astype(jnp.float32)
        before = jnp.where(me > 0, halo_before[s].astype(jnp.float32)[edge - 1 : edge], 0.0)
        after = jnp.where(me < devices - 1, halo_after[s].astype(jnp.float32)[:1], 0.0)
        previous = jnp.where(row == 0, before, pltpu.roll(middle, 1, 0))
        following = jnp.where(row == positions - 1, after, pltpu.roll(middle, positions - 1, 0))
        smoothed.append(
            short_ref[s, 0:1] * previous + short_ref[s, 1:2] * middle + short_ref[s, 2:3] * following
        )
    gated = smoothed[2] * smoothed[1]
    gated_send[...] = jnp.transpose(gated).astype(jnp.bfloat16).reshape(devices, share, positions)
    gated_recv[me] = gated_send[me]
    gated_copies = exchange(1, lambda device: gated_send.at[device], gated_recv.at[me])

    groups = devices + 1
    rows = groups * share
    shape = (groups, share, positions)
    cos_table = jnp.broadcast_to(twiddle_ref[0], shape).reshape(rows, positions)
    sin_table = jnp.broadcast_to(twiddle_ref[1], shape).reshape(rows, positions)
    inner_high, inner_low = inner_high_ref[...], inner_low_ref[...]

    def inner_product(operand, dims):
        high, low = split_pair(operand)
        return dot32(high, inner_high, dims) + (dot32(low, inner_high, dims) + dot32(high, inner_low, dims))

    def outer_product(operand):
        return dot32(outer_high[...], operand) + dot32(outer_low[...], operand)

    def spectrum(parts):
        blank = jnp.zeros((share, positions), jnp.float32)
        real_part = parts[:rows]
        imag_part = jnp.concatenate([blank, parts[rows:], blank], axis=0)
        turned_real = real_part * cos_table + imag_part * sin_table
        turned_imag = imag_part * cos_table - real_part * sin_table
        both = inner_product(jnp.concatenate([turned_real, turned_imag], axis=1), ((1,), (0,)))
        return both[:, :positions], both[:, positions:]

    loads[2].wait()
    loads[3].wait()
    for copy in taps_copies:
        copy.wait_recv()
    halves = jnp.concatenate(
        [taps_recv[half].reshape(devices * share, positions) for half in range(2)], axis=1
    )
    halves = outer_product(halves)
    part_row = lax.broadcasted_iota(jnp.int32, (2 * devices * share, positions), 0) // share
    frequency = jnp.where(part_row > devices, part_row - devices, part_row)
    second = halves[:, positions:]
    kernel_parts = halves[:, :positions] + jnp.where(frequency % 2 == 1, -second, second)
    kernel_real, kernel_imag = spectrum(kernel_parts)

    for copy in gated_copies:
        copy.wait_recv()
    signal_real, signal_imag = spectrum(outer_product(gated_recv[...].reshape(devices * share, positions)))
    product_real, product_imag = complex_times(signal_real, signal_imag, kernel_real, kernel_imag)
    both = inner_product(jnp.concatenate([product_real, product_imag], axis=1), ((1,), (1,)))
    real_part, imag_part = both[:, :positions], both[:, positions:]
    back_real = real_part * cos_table - imag_part * sin_table
    back_imag = real_part * sin_table + imag_part * cos_table
    scale = 1.0 / (2 * devices * positions)
    ends = lax.broadcasted_iota(jnp.int32, (rows, positions), 0) // share % devices == 0
    back_real = back_real * jnp.where(ends, scale, 2.0 * scale)
    back_imag = back_imag * (2.0 * scale)
    back = jnp.concatenate([back_real, back_imag[share : rows - share]], axis=0)
    high, low = split_pair(back)
    dims = ((0,), (0,))
    spatial = dot32(outer_high[...], high, dims) + (
        dot32(outer_high[...], low, dims) + dot32(outer_low[...], high, dims)
    )
    back_send[...] = spatial.astype(jnp.bfloat16).reshape(devices, share, positions)
    back_recv[me] = back_send[me]
    back_copies = exchange(2, lambda device: back_send.at[device], back_recv.at[me])
    for copy in back_copies:
        copy.wait_recv()
    convolved = jnp.transpose(back_recv[...].reshape(channels, positions).astype(jnp.float32))
    mixed = ((convolved + gain_ref[...] * gated) * smoothed[0]).astype(jnp.bfloat16)
    mean_square = jnp.mean(jnp.square(mixed.astype(jnp.float32)), axis=-1, keepdims=True)
    row_scale = lax.rsqrt(mean_square + EPSILON)
    loads[4].wait()
    out_ref[...] = (dot32(mixed, weight[...]) * row_scale).astype(jnp.bfloat16)
    for copy in taps_copies + gated_copies + back_copies:
        copy.wait_send()


def exchanged_once(axes, streams, filter_taps, short_taps, skip_gain, out_weight):
    positions, channels = streams.shape[2:]
    width = out_weight.shape[1]
    devices = lax.axis_size(axes[0]) * lax.axis_size(axes[1])
    share = channels // devices
    tables = host_tables(devices, share, positions)
    half = (devices, share, positions)
    edge = 16
    anywhere = pl.BlockSpec(memory_space=pl.ANY)
    vector = pl.BlockSpec(memory_space=pltpu.VMEM)
    outer_shape = tables[0].shape
    projected = pl.pallas_call(
        functools.partial(whole_kernel, axes, (devices, share, positions, channels)),
        out_shape=jax.ShapeDtypeStruct((positions, width), jnp.bfloat16),
        in_specs=[anywhere, anywhere, vector, vector, anywhere, anywhere, anywhere, vector, vector, vector],
        out_specs=vector,
        scratch_shapes=[
            pltpu.VMEM((3, positions, channels), jnp.bfloat16),
            pltpu.VMEM((2, positions, channels), jnp.float32),
            pltpu.VMEM((channels, width), jnp.bfloat16),
            pltpu.VMEM(outer_shape, jnp.bfloat16),
            pltpu.VMEM(outer_shape, jnp.bfloat16),
            pltpu.VMEM((3, edge, channels), jnp.bfloat16),
            pltpu.VMEM((3, edge, channels), jnp.bfloat16),
            pltpu.VMEM((2, *half), jnp.bfloat16),
            pltpu.VMEM((2, *half), jnp.bfloat16),
            pltpu.VMEM(half, jnp.bfloat16),
            pltpu.VMEM(half, jnp.bfloat16),
            pltpu.VMEM(half, jnp.bfloat16),
            pltpu.VMEM(half, jnp.bfloat16),
            pltpu.SemaphoreType.DMA((5,)),
            pltpu.SemaphoreType.DMA((4,)),
            pltpu.SemaphoreType.DMA((3, devices)),
            pltpu.SemaphoreType.DMA((3, devices)),
        ],
        compiler_params=pltpu.CompilerParams(collective_id=0, has_side_effects=True),
    )(
        streams.reshape(3, positions, channels),
        filter_taps,
        short_taps,
        skip_gain.reshape(1, channels),
        out_weight,
        *(jnp.asarray(table) for table in tables),
    )
    return projected.reshape(1, positions, width)


def local_any(axes, streams, *others):
    sequences, positions, channels = streams.shape[1:]
    devices = lax.axis_size(axes[0]) * lax.axis_size(axes[1])
    tiled = channels % (16 * devices) == 0 and positions == 128 and devices * channels <= 2**15
    if sequences == 1 and tiled and devices > 1:
        return exchanged_once(axes, streams, *others)
    return local(streams, *others)


def solution(mesh):
    in_specs = (P(None, None, ("row", "col"), None), P(None, ("row", "col"), None), P(), P(), P())
    out_specs = P(None, ("row", "col"), None)
    body = functools.partial(local_any, ("row", "col"))
    return jax.shard_map(body, mesh=mesh, in_specs=in_specs, out_specs=out_specs, check_vma=False)
```

```python
import functools
import math

import jax
import jax.numpy as jnp
import numpy as np
from jax import lax
from jax.experimental import pallas as pl
from jax.experimental.pallas import tpu as pltpu
from jax.sharding import PartitionSpec as P

HIGHEST_PRECISION = lax.Precision.HIGHEST
EPSILON = 1e-06


def with_halo(cells, sides, width):
    for axis, dim in sides:
        count = lax.axis_size(axis)
        ends = count - 1
        head = lax.slice_in_dim(cells, 0, width, axis=dim)
        tail = lax.slice_in_dim(cells, cells.shape[dim] - width, cells.shape[dim], axis=dim)
        cells = jnp.concatenate(
            [
                lax.ppermute(tail, axis, [(i, (i + 1) % count) for i in range(ends)]),
                cells,
                lax.ppermute(head, axis, [((i + 1) % count, i) for i in range(ends)]),
            ],
            axis=dim,
        )
    return cells


def unit_circle(numerator, period):
    angles = 2.0 * math.pi / period * (numerator % period).astype(jnp.float32)
    return (jnp.cos(angles), jnp.sin(angles))


def complex_times(left_real, left_imag, right_real, right_imag):
    return (
        left_real * right_real - left_imag * right_imag,
        left_real * right_imag + left_imag * right_real,
    )


def complex_einsum(formula, matrix_real, matrix_imag, operand_real, operand_imag):

    def single(matrix, operand):
        return jnp.einsum(formula, matrix, operand, precision=HIGHEST_PRECISION)

    return (
        single(matrix_real, operand_real) - single(matrix_imag, operand_imag),
        single(matrix_real, operand_imag) + single(matrix_imag, operand_real),
    )


def sequence_offsets(column_count, positions):
    blocks = jnp.arange(column_count, dtype=jnp.int32)
    within = jnp.arange(positions, dtype=jnp.int32)
    return (blocks, within, positions * blocks[:, None] + within[None, :])


def forward_rows(real_part, imag_part, frequencies, length):
    column_count, positions = (real_part.shape[1], real_part.shape[4])
    blocks, within, offsets = sequence_offsets(column_count, positions)
    cos_table, sin_table = unit_circle(frequencies[:, None, None] * offsets[None], length)
    real_part, imag_part = complex_times(
        real_part, imag_part, cos_table[:, :, None, None, :], -sin_table[:, :, None, None, :]
    )
    cos_table, sin_table = unit_circle(blocks[:, None] * blocks[None, :], column_count)
    real_part, imag_part = complex_einsum(
        "mc,rcbhj->rmbhj", cos_table, -sin_table, real_part, imag_part
    )
    cos_table, sin_table = unit_circle(blocks[:, None] * within[None, :], column_count * positions)
    real_part, imag_part = complex_times(
        real_part, imag_part, cos_table[None, :, None, None, :], -sin_table[None, :, None, None, :]
    )
    cos_table, sin_table = unit_circle(within[:, None] * within[None, :], positions)
    return complex_einsum("nj,rmbhj->rmbhn", cos_table, -sin_table, real_part, imag_part)


def inverse_rows(real_part, imag_part, frequencies, length):
    column_count, positions = (real_part.shape[1], real_part.shape[4])
    blocks, within, offsets = sequence_offsets(column_count, positions)
    cos_table, sin_table = unit_circle(within[:, None] * within[None, :], positions)
    real_part, imag_part = complex_einsum(
        "jn,rmbhn->rmbhj", cos_table, sin_table, real_part, imag_part
    )
    cos_table, sin_table = unit_circle(blocks[:, None] * within[None, :], column_count * positions)
    real_part, imag_part = complex_times(
        real_part, imag_part, cos_table[None, :, None, None, :], sin_table[None, :, None, None, :]
    )
    cos_table, sin_table = unit_circle(blocks[:, None] * blocks[None, :], column_count)
    real_part, imag_part = complex_einsum(
        "cm,rmbhj->rcbhj", cos_table, sin_table, real_part, imag_part
    )
    cos_table, sin_table = unit_circle(frequencies[:, None, None] * offsets[None], length)
    return complex_times(
        real_part, imag_part, cos_table[:, :, None, None, :], sin_table[:, :, None, None, :]
    )


def row_transform(operand, frequencies, sources, period):
    cos_table, sin_table = unit_circle(frequencies[:, None] * sources[None, :], period)
    imag_matrix = -sin_table
    flipped = unit_circle(period // 2 * sources[None, :], period)[0]
    imag_matrix = jnp.where(frequencies[:, None] == 0, flipped, imag_matrix)
    return (
        jnp.dot(cos_table, operand, precision=HIGHEST_PRECISION),
        jnp.dot(imag_matrix, operand, precision=HIGHEST_PRECISION),
    )


def row_inverse(real_part, imag_part, frequencies, rows_count, period, length):
    targets = jnp.arange(rows_count, dtype=jnp.int32)
    cos_table, sin_table = unit_circle(targets[:, None] * frequencies[None, :], period)
    real_matrix = cos_table / length
    imag_matrix = -sin_table / length
    flipped = unit_circle(period // 2 * targets[:, None], period)[0]
    head_row = frequencies[None, :] == 0
    real_matrix = jnp.where(head_row, 1.0, 2.0 * cos_table) / length
    imag_matrix = jnp.where(head_row, flipped, -2.0 * sin_table) / length
    return jnp.dot(real_matrix, real_part, precision=HIGHEST_PRECISION) + jnp.dot(
        imag_matrix, imag_part, precision=HIGHEST_PRECISION
    )


def unpack_head(real_part, imag_part, first_device):
    head_row = (jnp.arange(real_part.shape[0]) == 0)[:, None, None, None, None] & first_device
    extra_row = jnp.where(first_device, imag_part[:1], 0.0)
    cleared = jnp.where(head_row, 0.0, imag_part)
    return (
        jnp.concatenate([real_part, extra_row], axis=0),
        jnp.concatenate([cleared, jnp.zeros_like(extra_row)], axis=0),
    )


def pack_head(real_part, imag_part, first_device):
    head_imag = jnp.where(first_device, real_part[-1:], imag_part[:1])
    return (real_part[:-1], jnp.concatenate([head_imag, imag_part[1:-1]], axis=0))


def spectral_middle(signal, kernel, sequences, positions, share, column_index, send_out, send_back):
    rows_count = signal.shape[0]
    period = 2 * rows_count
    column_count = lax.axis_size("col")
    length = period * column_count * positions
    local_rows = rows_count // column_count
    frequencies = jnp.arange(rows_count, dtype=jnp.int32)
    signal_sources = jnp.arange(rows_count, dtype=jnp.int32)
    kernel_index = jnp.arange(period, dtype=jnp.int32)
    kernel_sources = kernel_index % 2 * rows_count + kernel_index // 2
    signal_real, signal_imag = row_transform(signal, frequencies, signal_sources, period)
    kernel_real, kernel_imag = row_transform(kernel, frequencies, kernel_sources, period)
    moved = send_out(
        signal_real[:, None], signal_imag[:, None], kernel_real[:, None], kernel_imag[:, None]
    )
    signal_shape = (local_rows, column_count, sequences, share, positions)
    kernel_shape = (local_rows, column_count, 1, share, positions)
    signal_real = moved[0].reshape(signal_shape)
    signal_imag = moved[1].reshape(signal_shape)
    kernel_real = moved[2].reshape(kernel_shape)
    kernel_imag = moved[3].reshape(kernel_shape)
    local_freq = column_index * local_rows + jnp.arange(local_rows, dtype=jnp.int32)
    first_device = column_index == 0
    signal_real, signal_imag = unpack_head(signal_real, signal_imag, first_device)
    kernel_real, kernel_imag = unpack_head(kernel_real, kernel_imag, first_device)
    local_freq = jnp.concatenate([local_freq, jnp.full((1,), rows_count, jnp.int32)])
    signal_real, signal_imag = forward_rows(signal_real, signal_imag, local_freq, length)
    kernel_real, kernel_imag = forward_rows(kernel_real, kernel_imag, local_freq, length)
    product_real, product_imag = complex_times(signal_real, signal_imag, kernel_real, kernel_imag)
    product_real, product_imag = inverse_rows(product_real, product_imag, local_freq, length)
    product_real, product_imag = pack_head(product_real, product_imag, first_device)
    returned = send_back(product_real, product_imag)
    columns = sequences * share * positions
    return row_inverse(
        returned[0].reshape(rows_count, columns),
        returned[1].reshape(rows_count, columns),
        frequencies,
        rows_count,
        period,
        length,
    )


def local(streams, filter_taps, short_taps, skip_gain, out_weight):
    sequences, positions, channels = (streams.shape[1], streams.shape[2], streams.shape[3])
    rows_count = lax.axis_size("row")
    share = channels // rows_count
    column_index = lax.axis_index("col")
    padded = with_halo(streams, ((("row", "col"), 2),), 1)
    smoothed = (
        short_taps[:, 0][:, None, None, :] * padded[:, :, :-2]
        + short_taps[:, 1][:, None, None, :] * padded[:, :, 1:-1]
        + short_taps[:, 2][:, None, None, :] * padded[:, :, 2:]
    )
    gated = smoothed[2] * smoothed[1]
    gated_lanes = jnp.transpose(gated, (0, 2, 1))[None]
    taps_lanes = jnp.transpose(filter_taps, (0, 2, 1))[:, None]
    by_channel, kernel_channel = (
        lax.all_to_all(gated_lanes, "row", split_axis=2, concat_axis=0, tiled=True),
        lax.all_to_all(taps_lanes, "row", split_axis=2, concat_axis=0, tiled=True),
    )
    signal = by_channel.reshape(rows_count, sequences * share * positions)
    kernel = kernel_channel.reshape(2 * rows_count, share * positions)

    def send_out(part_one, part_two, part_three, part_four):
        return (
            lax.all_to_all(part_one, "col", split_axis=0, concat_axis=1, tiled=True),
            lax.all_to_all(part_two, "col", split_axis=0, concat_axis=1, tiled=True),
            lax.all_to_all(part_three, "col", split_axis=0, concat_axis=1, tiled=True),
            lax.all_to_all(part_four, "col", split_axis=0, concat_axis=1, tiled=True),
        )

    def send_back(part_one, part_two):
        return (
            lax.all_to_all(part_one, "col", split_axis=1, concat_axis=0, tiled=True),
            lax.all_to_all(part_two, "col", split_axis=1, concat_axis=0, tiled=True),
        )

    spatial = spectral_middle(
        signal, kernel, sequences, positions, share, column_index, send_out, send_back
    )
    returned = lax.all_to_all(
        spatial.reshape(rows_count, sequences, share, positions),
        "row",
        split_axis=0,
        concat_axis=2,
        tiled=True,
    )
    convolved = jnp.transpose(returned[0], (0, 2, 1))
    mixed = ((convolved + skip_gain * gated) * smoothed[0]).astype(jnp.bfloat16)
    flattened = mixed.reshape(sequences * positions, channels)
    mean_square = jnp.mean(jnp.square(flattened.astype(jnp.float32)), axis=-1, keepdims=True)
    product = jnp.dot(flattened, out_weight, preferred_element_type=jnp.float32)
    scaled = (product * lax.rsqrt(mean_square + EPSILON)).astype(jnp.bfloat16)
    return scaled.reshape(sequences, positions, out_weight.shape[1])


def split_pair(value):
    high = value.astype(jnp.bfloat16)
    return high, (value - high.astype(jnp.float32)).astype(jnp.bfloat16)


def split_pair_host(table):
    table = np.asarray(table, np.float32)
    high = table.astype(jnp.bfloat16)
    return high, (table - high.astype(np.float32)).astype(jnp.bfloat16)


def host_tables(devices, share, positions):
    blocks = 2 * devices
    length = blocks * positions
    first = np.arange(devices + 1)
    source = np.arange(devices)
    angle = 2.0 * np.pi / blocks * (first[:, None] * source[None, :] % blocks)
    rows = np.concatenate([np.cos(angle), -np.sin(angle[1:devices])])
    outer = np.kron(rows, np.eye(share))
    within = np.arange(positions)
    angle = 2.0 * np.pi / length * (first[:, None] * within[None, :] % length)
    twiddle = np.stack([np.cos(angle), np.sin(angle)])[:, :, None, :].astype(np.float32)
    angle = 2.0 * np.pi / positions * (within[:, None] * within[None, :] % positions)
    cos_table, sin_table = np.cos(angle), np.sin(angle)
    inner = np.block([[cos_table, -sin_table], [sin_table, cos_table]])
    return (*split_pair_host(outer), *split_pair_host(inner), twiddle)


def dot32(left, right, dims=((1,), (0,))):
    return lax.dot_general(left, right, (dims, ((), ())), preferred_element_type=jnp.float32)


def whole_kernel(
    axes, sizes, streams_hbm, taps_hbm, short_hbm, gain_hbm, outer_high_hbm, outer_low_hbm,
    inner_high_hbm, inner_low_hbm, twiddle_hbm, weight_hbm, mixed_ref, scale_ref, weight_ref,
    streams, taps, short_ref, gain_ref, outer_high, outer_low, inner_high_ref, inner_low_ref, twiddle_ref,
    edges, halo_before, halo_after,
    taps_send, taps_recv, gated_send, gated_recv, back_send, back_recv,
    local_sems, halo_sems, send_sems, recv_sems,
):
    devices, share, positions, channels = sizes
    columns = lax.axis_size(axes[1])
    me = lax.axis_index(axes[0]) * columns + lax.axis_index(axes[1])
    mesh_id = pl.DeviceIdType.MESH

    def place(device):
        return (lax.div(device, columns), lax.rem(device, columns))

    def partner(step):
        return lax.rem(me + step, devices)

    loads = [
        pltpu.make_async_copy(source, target, local_sems.at[i])
        for i, (source, target) in enumerate(
            [
                (taps_hbm, taps),
                (streams_hbm, streams),
                (short_hbm, short_ref),
                (outer_high_hbm, outer_high),
                (outer_low_hbm, outer_low),
                (inner_high_hbm, inner_high_ref),
                (inner_low_hbm, inner_low_ref),
                (twiddle_hbm, twiddle_ref),
                (gain_hbm, gain_ref),
                (weight_hbm, weight_ref),
            ]
        )
    ]
    barrier = pltpu.get_barrier_semaphore()
    for load in loads[:3]:
        load.start()
    for step in range(1, devices):
        pl.semaphore_signal(barrier, inc=1, device_id=place(partner(step)), device_id_type=mesh_id)
    for load in loads[3:]:
        load.start()

    loads[0].wait()
    for half in range(2):
        turned = jnp.transpose(taps[half]).astype(jnp.bfloat16)
        taps_send[half] = turned.reshape(devices, share, positions)
    taps_recv[:, me] = taps_send[:, me]
    loads[1].wait()
    for s in range(3):
        middle = streams[s].astype(jnp.float32)
        edges[0, s : s + 1] = middle[positions - 1 :]
        edges[1, s : s + 1] = middle[:1]
    pl.semaphore_wait(barrier, devices - 1)

    halo_copies = [
        pltpu.make_async_remote_copy(
            src_ref=edges.at[side],
            dst_ref=halo,
            send_sem=halo_sems.at[2 * side],
            recv_sem=halo_sems.at[2 * side + 1],
            device_id=place(partner(step)),
            device_id_type=mesh_id,
        )
        for side, halo, step in ((0, halo_before, 1), (1, halo_after, devices - 1))
    ]
    for copy in halo_copies:
        copy.start()

    def exchange(kind, source, target):
        copies = []
        for step in range(1, devices):
            device = partner(step)
            copies.append(
                pltpu.make_async_remote_copy(
                    src_ref=source(device),
                    dst_ref=target,
                    send_sem=send_sems.at[kind, step],
                    recv_sem=recv_sems.at[kind, step],
                    device_id=place(device),
                    device_id_type=mesh_id,
                )
            )
        for copy in copies:
            copy.start()
        return copies

    taps_copies = exchange(0, lambda device: taps_send.at[:, device], taps_recv.at[:, me])

    loads[2].wait()
    for copy in halo_copies:
        copy.wait()
    row = lax.broadcasted_iota(jnp.int32, (positions, channels), 0)
    smoothed = []
    for s in range(3):
        middle = streams[s].astype(jnp.float32)
        before = jnp.where(me > 0, halo_before[s : s + 1], 0.0)
        after = jnp.where(me < devices - 1, halo_after[s : s + 1], 0.0)
        previous = jnp.where(row == 0, before, pltpu.roll(middle, 1, 0))
        following = jnp.where(row == positions - 1, after, pltpu.roll(middle, positions - 1, 0))
        smoothed.append(
            short_ref[s, 0:1] * previous + short_ref[s, 1:2] * middle + short_ref[s, 2:3] * following
        )
    gated = smoothed[2] * smoothed[1]
    gated_send[...] = jnp.transpose(gated).astype(jnp.bfloat16).reshape(devices, share, positions)
    gated_recv[me] = gated_send[me]
    gated_copies = exchange(1, lambda device: gated_send.at[device], gated_recv.at[me])

    for load in loads[3:9]:
        load.wait()
    groups = devices + 1
    rows = groups * share
    shape = (groups, share, positions)
    cos_table = jnp.broadcast_to(twiddle_ref[0], shape).reshape(rows, positions)
    sin_table = jnp.broadcast_to(twiddle_ref[1], shape).reshape(rows, positions)
    inner_high, inner_low = inner_high_ref[...], inner_low_ref[...]

    def inner_product(operand, dims):
        high, low = split_pair(operand)
        return dot32(high, inner_high, dims) + (dot32(low, inner_high, dims) + dot32(high, inner_low, dims))

    def outer_product(operand):
        return dot32(outer_high[...], operand) + dot32(outer_low[...], operand)

    def spectrum(parts):
        blank = jnp.zeros((share, positions), jnp.float32)
        real_part = parts[:rows]
        imag_part = jnp.concatenate([blank, parts[rows:], blank], axis=0)
        turned_real = real_part * cos_table + imag_part * sin_table
        turned_imag = imag_part * cos_table - real_part * sin_table
        both = inner_product(jnp.concatenate([turned_real, turned_imag], axis=1), ((1,), (0,)))
        return both[:, :positions], both[:, positions:]

    for copy in taps_copies:
        copy.wait_recv()
    halves = jnp.concatenate(
        [taps_recv[half].reshape(devices * share, positions) for half in range(2)], axis=1
    )
    halves = outer_product(halves)
    part_row = lax.broadcasted_iota(jnp.int32, (2 * devices * share, positions), 0) // share
    frequency = jnp.where(part_row > devices, part_row - devices, part_row)
    second = halves[:, positions:]
    kernel_parts = halves[:, :positions] + jnp.where(frequency % 2 == 1, -second, second)
    kernel_real, kernel_imag = spectrum(kernel_parts)

    for copy in gated_copies:
        copy.wait_recv()
    signal_real, signal_imag = spectrum(outer_product(gated_recv[...].reshape(devices * share, positions)))
    product_real, product_imag = complex_times(signal_real, signal_imag, kernel_real, kernel_imag)
    both = inner_product(jnp.concatenate([product_real, product_imag], axis=1), ((1,), (1,)))
    real_part, imag_part = both[:, :positions], both[:, positions:]
    back_real = real_part * cos_table - imag_part * sin_table
    back_imag = real_part * sin_table + imag_part * cos_table
    scale = 1.0 / (2 * devices * positions)
    ends = lax.broadcasted_iota(jnp.int32, (rows, positions), 0) // share % devices == 0
    back_real = back_real * jnp.where(ends, scale, 2.0 * scale)
    back_imag = back_imag * (2.0 * scale)
    back = jnp.concatenate([back_real, back_imag[share : rows - share]], axis=0)
    high, low = split_pair(back)
    dims = ((0,), (0,))
    spatial = dot32(outer_high[...], high, dims) + (
        dot32(outer_high[...], low, dims) + dot32(outer_low[...], high, dims)
    )
    back_send[...] = spatial.astype(jnp.bfloat16).reshape(devices, share, positions)
    back_recv[me] = back_send[me]
    back_copies = exchange(2, lambda device: back_send.at[device], back_recv.at[me])
    for copy in back_copies:
        copy.wait_recv()
    convolved = jnp.transpose(back_recv[...].reshape(channels, positions).astype(jnp.float32))
    mixed = ((convolved + gain_ref[...] * gated) * smoothed[0]).astype(jnp.bfloat16)
    mean_square = jnp.mean(jnp.square(mixed.astype(jnp.float32)), axis=-1, keepdims=True)
    mixed_ref[...] = mixed
    loads[9].wait()
    scale_ref[...] = lax.rsqrt(mean_square + EPSILON)
    for copy in taps_copies + gated_copies + back_copies:
        copy.wait_send()


def exchanged_once(axes, streams, filter_taps, short_taps, skip_gain, out_weight):
    positions, channels = streams.shape[2:]
    width = out_weight.shape[1]
    devices = lax.axis_size(axes[0]) * lax.axis_size(axes[1])
    share = channels // devices
    tables = host_tables(devices, share, positions)
    half = (devices, share, positions)
    anywhere = pl.BlockSpec(memory_space=pl.ANY)
    vector = pl.BlockSpec(memory_space=pltpu.VMEM)
    operands = (
        streams.reshape(3, positions, channels),
        filter_taps,
        short_taps,
        skip_gain.reshape(1, channels),
        *(jnp.asarray(table) for table in tables),
        out_weight,
    )

    def held(operand):
        return pltpu.VMEM(operand.shape, operand.dtype)

    mixed, row_scale, resident = pl.pallas_call(
        functools.partial(whole_kernel, axes, (devices, share, positions, channels)),
        out_shape=[
            pltpu.VMEM((positions, channels), jnp.bfloat16),
            pltpu.VMEM((positions, 1), jnp.float32),
            held(out_weight),
        ],
        in_specs=[anywhere] * len(operands),
        out_specs=[vector, vector, vector],
        scratch_shapes=[
            *(held(operand) for operand in operands[:-1]),
            pltpu.VMEM((2, 8, channels), jnp.float32),
            pltpu.VMEM((8, channels), jnp.float32),
            pltpu.VMEM((8, channels), jnp.float32),
            pltpu.VMEM((2, *half), jnp.bfloat16),
            pltpu.VMEM((2, *half), jnp.bfloat16),
            pltpu.VMEM(half, jnp.bfloat16),
            pltpu.VMEM(half, jnp.bfloat16),
            pltpu.VMEM(half, jnp.bfloat16),
            pltpu.VMEM(half, jnp.bfloat16),
            pltpu.SemaphoreType.DMA((len(operands),)),
            pltpu.SemaphoreType.DMA((4,)),
            pltpu.SemaphoreType.DMA((3, devices)),
            pltpu.SemaphoreType.DMA((3, devices)),
        ],
        compiler_params=pltpu.CompilerParams(
            collective_id=0, has_side_effects=True, vmem_limit_bytes=24 * 2**20
        ),
        cost_estimate=pl.CostEstimate(flops=10**10, bytes_accessed=10**7, transcendentals=0),
    )(*(pltpu.with_memory_space_constraint(operand, pltpu.HBM) for operand in operands))
    chunks = 8
    chunk = width // chunks

    def project(mixed_ref, scale_ref, weight_ref, out_hbm, out_tiles, sems):
        for i in range(chunks):
            columns = pl.ds(i * chunk, chunk)
            value = dot32(mixed_ref[...], weight_ref[:, columns]) * scale_ref[...]
            out_tiles[:, columns] = value.astype(jnp.bfloat16)
            pltpu.make_async_copy(out_tiles.at[:, columns], out_hbm.at[:, columns], sems.at[i]).start()
        for i in range(chunks):
            columns = pl.ds(i * chunk, chunk)
            pltpu.make_async_copy(out_tiles.at[:, columns], out_hbm.at[:, columns], sems.at[i]).wait()

    projected = pl.pallas_call(
        project,
        out_shape=jax.ShapeDtypeStruct((positions, width), jnp.bfloat16),
        in_specs=[vector] * 3,
        out_specs=anywhere,
        scratch_shapes=[
            pltpu.VMEM((positions, width), jnp.bfloat16),
            pltpu.SemaphoreType.DMA((chunks,)),
        ],
        compiler_params=pltpu.CompilerParams(vmem_limit_bytes=16 * 2**20),
    )(*(pltpu.with_memory_space_constraint(held_value, pltpu.VMEM) for held_value in (mixed, row_scale, resident)))
    return projected.reshape(1, positions, width)


def local_any(axes, streams, *others):
    sequences, positions, channels = streams.shape[1:]
    devices = lax.axis_size(axes[0]) * lax.axis_size(axes[1])
    tiled = channels % (16 * devices) == 0 and positions == 128 and devices * channels <= 2**15
    if sequences == 1 and tiled and devices > 1:
        return exchanged_once(axes, streams, *others)
    return local(streams, *others)


def solution(mesh):
    in_specs = (P(None, None, ("row", "col"), None), P(None, ("row", "col"), None), P(), P(), P())
    out_specs = P(None, ("row", "col"), None)
    body = functools.partial(local_any, ("row", "col"))
    return jax.shard_map(body, mesh=mesh, in_specs=in_specs, out_specs=out_specs, check_vma=False)
```

```python
import functools
import math

import jax
import jax.numpy as jnp
import numpy as np
from jax import lax
from jax.experimental import pallas as pl
from jax.experimental.pallas import tpu as pltpu
from jax.sharding import PartitionSpec as P

HIGHEST_PRECISION = lax.Precision.HIGHEST
EPSILON = 1e-06


def with_halo(cells, sides, width):
    for axis, dim in sides:
        count = lax.axis_size(axis)
        ends = count - 1
        head = lax.slice_in_dim(cells, 0, width, axis=dim)
        tail = lax.slice_in_dim(cells, cells.shape[dim] - width, cells.shape[dim], axis=dim)
        cells = jnp.concatenate(
            [
                lax.ppermute(tail, axis, [(i, (i + 1) % count) for i in range(ends)]),
                cells,
                lax.ppermute(head, axis, [((i + 1) % count, i) for i in range(ends)]),
            ],
            axis=dim,
        )
    return cells


def unit_circle(numerator, period):
    angles = 2.0 * math.pi / period * (numerator % period).astype(jnp.float32)
    return (jnp.cos(angles), jnp.sin(angles))


def complex_times(left_real, left_imag, right_real, right_imag):
    return (
        left_real * right_real - left_imag * right_imag,
        left_real * right_imag + left_imag * right_real,
    )


def complex_einsum(formula, matrix_real, matrix_imag, operand_real, operand_imag):

    def single(matrix, operand):
        return jnp.einsum(formula, matrix, operand, precision=HIGHEST_PRECISION)

    return (
        single(matrix_real, operand_real) - single(matrix_imag, operand_imag),
        single(matrix_real, operand_imag) + single(matrix_imag, operand_real),
    )


def sequence_offsets(column_count, positions):
    blocks = jnp.arange(column_count, dtype=jnp.int32)
    within = jnp.arange(positions, dtype=jnp.int32)
    return (blocks, within, positions * blocks[:, None] + within[None, :])


def forward_rows(real_part, imag_part, frequencies, length):
    column_count, positions = (real_part.shape[1], real_part.shape[4])
    blocks, within, offsets = sequence_offsets(column_count, positions)
    cos_table, sin_table = unit_circle(frequencies[:, None, None] * offsets[None], length)
    real_part, imag_part = complex_times(
        real_part, imag_part, cos_table[:, :, None, None, :], -sin_table[:, :, None, None, :]
    )
    cos_table, sin_table = unit_circle(blocks[:, None] * blocks[None, :], column_count)
    real_part, imag_part = complex_einsum(
        "mc,rcbhj->rmbhj", cos_table, -sin_table, real_part, imag_part
    )
    cos_table, sin_table = unit_circle(blocks[:, None] * within[None, :], column_count * positions)
    real_part, imag_part = complex_times(
        real_part, imag_part, cos_table[None, :, None, None, :], -sin_table[None, :, None, None, :]
    )
    cos_table, sin_table = unit_circle(within[:, None] * within[None, :], positions)
    return complex_einsum("nj,rmbhj->rmbhn", cos_table, -sin_table, real_part, imag_part)


def inverse_rows(real_part, imag_part, frequencies, length):
    column_count, positions = (real_part.shape[1], real_part.shape[4])
    blocks, within, offsets = sequence_offsets(column_count, positions)
    cos_table, sin_table = unit_circle(within[:, None] * within[None, :], positions)
    real_part, imag_part = complex_einsum(
        "jn,rmbhn->rmbhj", cos_table, sin_table, real_part, imag_part
    )
    cos_table, sin_table = unit_circle(blocks[:, None] * within[None, :], column_count * positions)
    real_part, imag_part = complex_times(
        real_part, imag_part, cos_table[None, :, None, None, :], sin_table[None, :, None, None, :]
    )
    cos_table, sin_table = unit_circle(blocks[:, None] * blocks[None, :], column_count)
    real_part, imag_part = complex_einsum(
        "cm,rmbhj->rcbhj", cos_table, sin_table, real_part, imag_part
    )
    cos_table, sin_table = unit_circle(frequencies[:, None, None] * offsets[None], length)
    return complex_times(
        real_part, imag_part, cos_table[:, :, None, None, :], sin_table[:, :, None, None, :]
    )


def row_transform(operand, frequencies, sources, period):
    cos_table, sin_table = unit_circle(frequencies[:, None] * sources[None, :], period)
    imag_matrix = -sin_table
    flipped = unit_circle(period // 2 * sources[None, :], period)[0]
    imag_matrix = jnp.where(frequencies[:, None] == 0, flipped, imag_matrix)
    return (
        jnp.dot(cos_table, operand, precision=HIGHEST_PRECISION),
        jnp.dot(imag_matrix, operand, precision=HIGHEST_PRECISION),
    )


def row_inverse(real_part, imag_part, frequencies, rows_count, period, length):
    targets = jnp.arange(rows_count, dtype=jnp.int32)
    cos_table, sin_table = unit_circle(targets[:, None] * frequencies[None, :], period)
    real_matrix = cos_table / length
    imag_matrix = -sin_table / length
    flipped = unit_circle(period // 2 * targets[:, None], period)[0]
    head_row = frequencies[None, :] == 0
    real_matrix = jnp.where(head_row, 1.0, 2.0 * cos_table) / length
    imag_matrix = jnp.where(head_row, flipped, -2.0 * sin_table) / length
    return jnp.dot(real_matrix, real_part, precision=HIGHEST_PRECISION) + jnp.dot(
        imag_matrix, imag_part, precision=HIGHEST_PRECISION
    )


def unpack_head(real_part, imag_part, first_device):
    head_row = (jnp.arange(real_part.shape[0]) == 0)[:, None, None, None, None] & first_device
    extra_row = jnp.where(first_device, imag_part[:1], 0.0)
    cleared = jnp.where(head_row, 0.0, imag_part)
    return (
        jnp.concatenate([real_part, extra_row], axis=0),
        jnp.concatenate([cleared, jnp.zeros_like(extra_row)], axis=0),
    )


def pack_head(real_part, imag_part, first_device):
    head_imag = jnp.where(first_device, real_part[-1:], imag_part[:1])
    return (real_part[:-1], jnp.concatenate([head_imag, imag_part[1:-1]], axis=0))


def spectral_middle(signal, kernel, sequences, positions, share, column_index, send_out, send_back):
    rows_count = signal.shape[0]
    period = 2 * rows_count
    column_count = lax.axis_size("col")
    length = period * column_count * positions
    local_rows = rows_count // column_count
    frequencies = jnp.arange(rows_count, dtype=jnp.int32)
    signal_sources = jnp.arange(rows_count, dtype=jnp.int32)
    kernel_index = jnp.arange(period, dtype=jnp.int32)
    kernel_sources = kernel_index % 2 * rows_count + kernel_index // 2
    signal_real, signal_imag = row_transform(signal, frequencies, signal_sources, period)
    kernel_real, kernel_imag = row_transform(kernel, frequencies, kernel_sources, period)
    moved = send_out(
        signal_real[:, None], signal_imag[:, None], kernel_real[:, None], kernel_imag[:, None]
    )
    signal_shape = (local_rows, column_count, sequences, share, positions)
    kernel_shape = (local_rows, column_count, 1, share, positions)
    signal_real = moved[0].reshape(signal_shape)
    signal_imag = moved[1].reshape(signal_shape)
    kernel_real = moved[2].reshape(kernel_shape)
    kernel_imag = moved[3].reshape(kernel_shape)
    local_freq = column_index * local_rows + jnp.arange(local_rows, dtype=jnp.int32)
    first_device = column_index == 0
    signal_real, signal_imag = unpack_head(signal_real, signal_imag, first_device)
    kernel_real, kernel_imag = unpack_head(kernel_real, kernel_imag, first_device)
    local_freq = jnp.concatenate([local_freq, jnp.full((1,), rows_count, jnp.int32)])
    signal_real, signal_imag = forward_rows(signal_real, signal_imag, local_freq, length)
    kernel_real, kernel_imag = forward_rows(kernel_real, kernel_imag, local_freq, length)
    product_real, product_imag = complex_times(signal_real, signal_imag, kernel_real, kernel_imag)
    product_real, product_imag = inverse_rows(product_real, product_imag, local_freq, length)
    product_real, product_imag = pack_head(product_real, product_imag, first_device)
    returned = send_back(product_real, product_imag)
    columns = sequences * share * positions
    return row_inverse(
        returned[0].reshape(rows_count, columns),
        returned[1].reshape(rows_count, columns),
        frequencies,
        rows_count,
        period,
        length,
    )


def local(streams, filter_taps, short_taps, skip_gain, out_weight):
    sequences, positions, channels = (streams.shape[1], streams.shape[2], streams.shape[3])
    rows_count = lax.axis_size("row")
    share = channels // rows_count
    column_index = lax.axis_index("col")
    padded = with_halo(streams, ((("row", "col"), 2),), 1)
    smoothed = (
        short_taps[:, 0][:, None, None, :] * padded[:, :, :-2]
        + short_taps[:, 1][:, None, None, :] * padded[:, :, 1:-1]
        + short_taps[:, 2][:, None, None, :] * padded[:, :, 2:]
    )
    gated = smoothed[2] * smoothed[1]
    gated_lanes = jnp.transpose(gated, (0, 2, 1))[None]
    taps_lanes = jnp.transpose(filter_taps, (0, 2, 1))[:, None]
    by_channel, kernel_channel = (
        lax.all_to_all(gated_lanes, "row", split_axis=2, concat_axis=0, tiled=True),
        lax.all_to_all(taps_lanes, "row", split_axis=2, concat_axis=0, tiled=True),
    )
    signal = by_channel.reshape(rows_count, sequences * share * positions)
    kernel = kernel_channel.reshape(2 * rows_count, share * positions)

    def send_out(part_one, part_two, part_three, part_four):
        return (
            lax.all_to_all(part_one, "col", split_axis=0, concat_axis=1, tiled=True),
            lax.all_to_all(part_two, "col", split_axis=0, concat_axis=1, tiled=True),
            lax.all_to_all(part_three, "col", split_axis=0, concat_axis=1, tiled=True),
            lax.all_to_all(part_four, "col", split_axis=0, concat_axis=1, tiled=True),
        )

    def send_back(part_one, part_two):
        return (
            lax.all_to_all(part_one, "col", split_axis=1, concat_axis=0, tiled=True),
            lax.all_to_all(part_two, "col", split_axis=1, concat_axis=0, tiled=True),
        )

    spatial = spectral_middle(
        signal, kernel, sequences, positions, share, column_index, send_out, send_back
    )
    returned = lax.all_to_all(
        spatial.reshape(rows_count, sequences, share, positions),
        "row",
        split_axis=0,
        concat_axis=2,
        tiled=True,
    )
    convolved = jnp.transpose(returned[0], (0, 2, 1))
    mixed = ((convolved + skip_gain * gated) * smoothed[0]).astype(jnp.bfloat16)
    flattened = mixed.reshape(sequences * positions, channels)
    mean_square = jnp.mean(jnp.square(flattened.astype(jnp.float32)), axis=-1, keepdims=True)
    product = jnp.dot(flattened, out_weight, preferred_element_type=jnp.float32)
    scaled = (product * lax.rsqrt(mean_square + EPSILON)).astype(jnp.bfloat16)
    return scaled.reshape(sequences, positions, out_weight.shape[1])


def split_pair(value):
    high = value.astype(jnp.bfloat16)
    return high, (value - high.astype(jnp.float32)).astype(jnp.bfloat16)


def split_pair_host(table):
    table = np.asarray(table, np.float32)
    high = table.astype(jnp.bfloat16)
    return high, (table - high.astype(np.float32)).astype(jnp.bfloat16)


def host_tables(devices, share, positions):
    blocks = 2 * devices
    length = blocks * positions
    first = np.arange(devices + 1)
    source = np.arange(devices)
    angle = 2.0 * np.pi / blocks * (first[:, None] * source[None, :] % blocks)
    rows = np.concatenate([np.cos(angle), -np.sin(angle[1:devices])])
    outer = np.kron(rows, np.eye(share))
    within = np.arange(positions)
    angle = 2.0 * np.pi / length * (first[:, None] * within[None, :] % length)
    twiddle = np.stack([np.cos(angle), np.sin(angle)])[:, :, None, :].astype(np.float32)
    angle = 2.0 * np.pi / positions * (within[:, None] * within[None, :] % positions)
    cos_table, sin_table = np.cos(angle), np.sin(angle)
    inner = np.block([[cos_table, -sin_table], [sin_table, cos_table]])
    return (*split_pair_host(outer), *split_pair_host(inner), twiddle)


def dot32(left, right, dims=((1,), (0,))):
    return lax.dot_general(left, right, (dims, ((), ())), preferred_element_type=jnp.float32)


def whole_kernel(
    axes, sizes, streams_hbm, taps_hbm, short_hbm, gain_hbm, outer_high_hbm, outer_low_hbm,
    inner_high_hbm, inner_low_hbm, twiddle_hbm, weight_hbm, mixed_ref, scale_ref, weight_ref,
    streams, taps, short_ref, gain_ref, outer_high, outer_low, inner_high_ref, inner_low_ref, twiddle_ref,
    turned_high, turned_low, edges, halo_before, halo_after,
    taps_send, taps_recv, gated_send, gated_recv, back_send, back_recv,
    local_sems, halo_sems, send_sems, recv_sems,
):
    devices, share, positions, channels = sizes
    columns = lax.axis_size(axes[1])
    me = lax.axis_index(axes[0]) * columns + lax.axis_index(axes[1])
    mesh_id = pl.DeviceIdType.MESH

    def place(device):
        return (lax.div(device, columns), lax.rem(device, columns))

    def partner(step):
        return lax.rem(me + step, devices)

    loads = [
        pltpu.make_async_copy(source, target, local_sems.at[i])
        for i, (source, target) in enumerate(
            [
                (taps_hbm, taps),
                (streams_hbm, streams),
                (short_hbm, short_ref),
                (outer_high_hbm, outer_high),
                (outer_low_hbm, outer_low),
                (inner_high_hbm, inner_high_ref),
                (inner_low_hbm, inner_low_ref),
                (twiddle_hbm, twiddle_ref),
                (gain_hbm, gain_ref),
                (weight_hbm, weight_ref),
            ]
        )
    ]
    barrier = pltpu.get_barrier_semaphore()
    for load in loads[:3]:
        load.start()
    for step in range(1, devices):
        pl.semaphore_signal(barrier, inc=1, device_id=place(partner(step)), device_id_type=mesh_id)
    for load in loads[3:]:
        load.start()

    loads[0].wait()
    for half in range(2):
        turned = jnp.transpose(taps[half]).astype(jnp.bfloat16)
        taps_send[:, half] = turned.reshape(devices, share, positions)
    taps_recv[me] = taps_send[me]
    loads[1].wait()
    for s in range(3):
        middle = streams[s].astype(jnp.float32)
        edges[0, s : s + 1] = middle[positions - 1 :]
        edges[1, s : s + 1] = middle[:1]
    pl.semaphore_wait(barrier, devices - 1)

    halo_copies = [
        pltpu.make_async_remote_copy(
            src_ref=edges.at[side],
            dst_ref=halo,
            send_sem=halo_sems.at[2 * side],
            recv_sem=halo_sems.at[2 * side + 1],
            device_id=place(partner(step)),
            device_id_type=mesh_id,
        )
        for side, halo, step in ((0, halo_before, 1), (1, halo_after, devices - 1))
    ]
    for copy in halo_copies:
        copy.start()

    def exchange(kind, source, target):
        copies = []
        for step in range(1, devices):
            device = partner(step)
            copies.append(
                pltpu.make_async_remote_copy(
                    src_ref=source(device),
                    dst_ref=target,
                    send_sem=send_sems.at[kind, step],
                    recv_sem=recv_sems.at[kind, step],
                    device_id=place(device),
                    device_id_type=mesh_id,
                )
            )
        for copy in copies:
            copy.start()
        return copies

    taps_copies = exchange(0, lambda device: taps_send.at[device], taps_recv.at[me])

    loads[2].wait()
    for copy in halo_copies:
        copy.wait()
    row = lax.broadcasted_iota(jnp.int32, (positions, channels), 0)
    smoothed = []
    for s in range(3):
        middle = streams[s].astype(jnp.float32)
        before = jnp.where(me > 0, halo_before[s : s + 1], 0.0)
        after = jnp.where(me < devices - 1, halo_after[s : s + 1], 0.0)
        previous = jnp.where(row == 0, before, pltpu.roll(middle, 1, 0))
        following = jnp.where(row == positions - 1, after, pltpu.roll(middle, positions - 1, 0))
        smoothed.append(
            short_ref[s, 0:1] * previous + short_ref[s, 1:2] * middle + short_ref[s, 2:3] * following
        )
    gated = smoothed[2] * smoothed[1]
    gated_send[...] = jnp.transpose(gated).astype(jnp.bfloat16).reshape(devices, share, positions)
    gated_recv[me] = gated_send[me]
    gated_copies = exchange(1, lambda device: gated_send.at[device], gated_recv.at[me])

    for load in loads[3:9]:
        load.wait()
    turned_high[...] = jnp.transpose(outer_high[...])
    turned_low[...] = jnp.transpose(outer_low[...])
    groups = devices + 1
    rows = groups * share
    shape = (groups, share, positions)
    cos_table = jnp.broadcast_to(twiddle_ref[0], shape).reshape(rows, positions)
    sin_table = jnp.broadcast_to(twiddle_ref[1], shape).reshape(rows, positions)
    inner_high, inner_low = inner_high_ref[...], inner_low_ref[...]

    def inner_product(operand, dims):
        high, low = split_pair(operand)
        return dot32(high, inner_high, dims) + (dot32(low, inner_high, dims) + dot32(high, inner_low, dims))

    def outer_product(operand):
        return dot32(outer_high[...], operand) + dot32(outer_low[...], operand)

    def spectrum(parts):
        blank = jnp.zeros((share, positions), jnp.float32)
        real_part = parts[:rows]
        imag_part = jnp.concatenate([blank, parts[rows:], blank], axis=0)
        turned_real = real_part * cos_table + imag_part * sin_table
        turned_imag = imag_part * cos_table - real_part * sin_table
        both = inner_product(jnp.concatenate([turned_real, turned_imag], axis=1), ((1,), (0,)))
        return both[:, :positions], both[:, positions:]

    for copy in taps_copies:
        copy.wait_recv()
    halves = jnp.concatenate(
        [taps_recv[:, half].reshape(devices * share, positions) for half in range(2)], axis=1
    )
    halves = outer_product(halves)
    part_row = lax.broadcasted_iota(jnp.int32, (2 * devices * share, positions), 0) // share
    frequency = jnp.where(part_row > devices, part_row - devices, part_row)
    second = halves[:, positions:]
    kernel_parts = halves[:, :positions] + jnp.where(frequency % 2 == 1, -second, second)
    kernel_real, kernel_imag = spectrum(kernel_parts)

    for copy in gated_copies:
        copy.wait_recv()
    signal_real, signal_imag = spectrum(dot32(outer_high[...], gated_recv[...].reshape(devices * share, positions)))
    product_real, product_imag = complex_times(signal_real, signal_imag, kernel_real, kernel_imag)
    both = inner_product(jnp.concatenate([product_real, product_imag], axis=1), ((1,), (1,)))
    real_part, imag_part = both[:, :positions], both[:, positions:]
    back_real = real_part * cos_table - imag_part * sin_table
    back_imag = real_part * sin_table + imag_part * cos_table
    scale = 1.0 / (2 * devices * positions)
    ends = lax.broadcasted_iota(jnp.int32, (rows, positions), 0) // share % devices == 0
    back_real = back_real * jnp.where(ends, scale, 2.0 * scale)
    back_imag = back_imag * (2.0 * scale)
    back = jnp.concatenate([back_real, back_imag[share : rows - share]], axis=0)
    high, low = split_pair(back)
    both = dot32(turned_high[...], jnp.concatenate([high, low], axis=1))
    spatial = both[:, :positions] + (both[:, positions:] + dot32(turned_low[...], high))
    back_send[...] = spatial.astype(jnp.bfloat16).reshape(devices, share, positions)
    back_recv[me] = back_send[me]
    back_copies = exchange(2, lambda device: back_send.at[device], back_recv.at[me])
    for copy in back_copies:
        copy.wait_recv()
    convolved = jnp.transpose(back_recv[...].reshape(channels, positions).astype(jnp.float32))
    mixed = ((convolved + gain_ref[...] * gated) * smoothed[0]).astype(jnp.bfloat16)
    mean_square = jnp.mean(jnp.square(mixed.astype(jnp.float32)), axis=-1, keepdims=True)
    mixed_ref[...] = mixed
    loads[9].wait()
    scale_ref[...] = lax.rsqrt(mean_square + EPSILON)
    for copy in taps_copies + gated_copies + back_copies:
        copy.wait_send()


def exchanged_once(axes, streams, filter_taps, short_taps, skip_gain, out_weight):
    positions, channels = streams.shape[2:]
    width = out_weight.shape[1]
    devices = lax.axis_size(axes[0]) * lax.axis_size(axes[1])
    share = channels // devices
    tables = host_tables(devices, share, positions)
    half = (devices, share, positions)
    anywhere = pl.BlockSpec(memory_space=pl.ANY)
    vector = pl.BlockSpec(memory_space=pltpu.VMEM)
    operands = (
        streams.reshape(3, positions, channels),
        filter_taps,
        short_taps,
        skip_gain.reshape(1, channels),
        *(jnp.asarray(table) for table in tables),
        out_weight,
    )

    def held(operand):
        return pltpu.VMEM(operand.shape, operand.dtype)

    mixed, row_scale, resident = pl.pallas_call(
        functools.partial(whole_kernel, axes, (devices, share, positions, channels)),
        out_shape=[
            pltpu.VMEM((positions, channels), jnp.bfloat16),
            pltpu.VMEM((positions, 1), jnp.float32),
            held(out_weight),
        ],
        in_specs=[anywhere] * len(operands),
        out_specs=[vector, vector, vector],
        scratch_shapes=[
            *(held(operand) for operand in operands[:-1]),
            pltpu.VMEM(tables[0].shape[::-1], jnp.bfloat16),
            pltpu.VMEM(tables[0].shape[::-1], jnp.bfloat16),
            pltpu.VMEM((2, 8, channels), jnp.float32),
            pltpu.VMEM((8, channels), jnp.float32),
            pltpu.VMEM((8, channels), jnp.float32),
            pltpu.VMEM((devices, 2, share, positions), jnp.bfloat16),
            pltpu.VMEM((devices, 2, share, positions), jnp.bfloat16),
            pltpu.VMEM(half, jnp.bfloat16),
            pltpu.VMEM(half, jnp.bfloat16),
            pltpu.VMEM(half, jnp.bfloat16),
            pltpu.VMEM(half, jnp.bfloat16),
            pltpu.SemaphoreType.DMA((len(operands),)),
            pltpu.SemaphoreType.DMA((4,)),
            pltpu.SemaphoreType.DMA((3, devices)),
            pltpu.SemaphoreType.DMA((3, devices)),
        ],
        compiler_params=pltpu.CompilerParams(
            collective_id=0, has_side_effects=True, vmem_limit_bytes=24 * 2**20
        ),
        cost_estimate=pl.CostEstimate(flops=10**10, bytes_accessed=10**7, transcendentals=0),
    )(*(pltpu.with_memory_space_constraint(operand, pltpu.HBM) for operand in operands))
    chunks = 8
    chunk = width // chunks

    def project(mixed_ref, scale_ref, weight_ref, out_hbm, out_tiles, sems):
        for i in range(chunks):
            columns = pl.ds(i * chunk, chunk)
            value = dot32(mixed_ref[...], weight_ref[:, columns]) * scale_ref[...]
            out_tiles[:, columns] = value.astype(jnp.bfloat16)
            pltpu.make_async_copy(out_tiles.at[:, columns], out_hbm.at[:, columns], sems.at[i]).start()
        for i in range(chunks):
            columns = pl.ds(i * chunk, chunk)
            pltpu.make_async_copy(out_tiles.at[:, columns], out_hbm.at[:, columns], sems.at[i]).wait()

    projected = pl.pallas_call(
        project,
        out_shape=jax.ShapeDtypeStruct((positions, width), jnp.bfloat16),
        in_specs=[vector] * 3,
        out_specs=anywhere,
        scratch_shapes=[
            pltpu.VMEM((positions, width), jnp.bfloat16),
            pltpu.SemaphoreType.DMA((chunks,)),
        ],
        compiler_params=pltpu.CompilerParams(vmem_limit_bytes=16 * 2**20),
    )(*(pltpu.with_memory_space_constraint(held_value, pltpu.VMEM) for held_value in (mixed, row_scale, resident)))
    return projected.reshape(1, positions, width)


def local_any(axes, streams, *others):
    sequences, positions, channels = streams.shape[1:]
    devices = lax.axis_size(axes[0]) * lax.axis_size(axes[1])
    tiled = channels % (16 * devices) == 0 and positions == 128 and devices * channels <= 2**15
    if sequences == 1 and tiled and devices > 1:
        return exchanged_once(axes, streams, *others)
    return local(streams, *others)


def solution(mesh):
    in_specs = (P(None, None, ("row", "col"), None), P(None, ("row", "col"), None), P(), P(), P())
    out_specs = P(None, ("row", "col"), None)
    body = functools.partial(local_any, ("row", "col"))
    return jax.shard_map(body, mesh=mesh, in_specs=in_specs, out_specs=out_specs, check_vma=False)
```
